32 devices in a mesh: kv: 8 (over z, y), tp: 4 (over x, core).
Axes of the slice: x: 2, y: 2, z: 4, core: 2. Of those that a mesh axis runs over, the one named last changes fastest.
Arguments:
- tokens: bfloat16 [16, 3072], P('kv', 'tp'), may hold values from -15 to 15
- associative_state: float32 [16, 16, 128, 128], P('kv', 'tp'), may hold values from -2 to 2
- sudden_extra_decay: float32 [16, 16], P('kv', 'tp'), may hold values from -0.7 to 0
- head_decay_speed: float32 [16], P('tp'), may hold values from 0.05 to 2
- opening_norm_gain: float32 [3072], P('tp'), may hold values from 0.1 to 1.9
- opening_gate_weight: bfloat16 [3072, 8448], P('tp', 'kv'), may hold values from -0.109375 to 0.109375
- opening_up_weight: bfloat16 [3072, 8448], P('tp', 'kv'), may hold values from -0.109375 to 0.109375
- opening_down_weight: bfloat16 [8448, 3072], P('kv', 'tp'), may hold values from -0.25 to 0.25
- mixer_norm_gain: float32 [3072], P('tp'), may hold values from 0.1 to 1.9
- query_matrix: bfloat16 [3072, 2048], P('tp'), may hold values from -0.109375 to 0.109375
- key_matrix: bfloat16 [3072, 2048], P('tp'), may hold values from -0.109375 to 0.109375
- value_matrix: bfloat16 [3072, 2048], P('tp'), may hold values from -0.109375 to 0.109375
- output_gate_matrix: bfloat16 [3072, 2048], P('tp'), may hold values from -0.109375 to 0.109375
- strength_weight: bfloat16 [3072, 16], P('tp'), may hold values from -0.109375 to 0.109375
- decay_matrix: bfloat16 [3072, 16], P('tp'), may hold values from -0.109375 to 0.109375
- head_read_gain: float32 [128], replicated, may hold values from 0.1 to 1.9
- output_matrix: bfloat16 [2048, 3072], P('tp'), may hold values from -0.125 to 0.125
- closing_norm_gain: float32 [3072], P('tp'), may hold values from 0.1 to 1.9
- closing_gate_weight: bfloat16 [3072, 8448], P('tp', 'kv'), may hold values from -0.109375 to 0.109375
- closing_up_weight: bfloat16 [3072, 8448], P('tp', 'kv'), may hold values from -0.109375 to 0.109375
- closing_down_weight: bfloat16 [8448, 3072], P('kv', 'tp'), may hold values from -0.25 to 0.25
Outputs:
- layer_out: bfloat16 [16, 3072], P('kv', 'tp')
- memory_new: float32 [16, 16, 128, 128], P('kv', 'tp')
The draws below stay inside these ranges and needn't reach their ends.
All inputs are finite; a program needn't handle non-finite values.
Results may differ from the reference program's by a relative error of at most 0.023.
Values may be sent and summed in bfloat16 or wider, within the bound.
A program may use at most 64 MiB of HBM per device.

```python
import math
import jax
import jax.numpy as jnp
from jax import lax

D = 3072
FF = 8448
MIXER_HEADS = 16
HEAD = 128
SEQUENCE_COUNT = 16
N_TP = 4


def draw_tokens(key, part):
    column = jnp.exp(jnp.log(3.0) * jnp.arange(D, dtype=jnp.float32) / D)
    values = jnp.clip(jax.random.normal(jax.random.fold_in(key, 1), (SEQUENCE_COUNT, D), jnp.float32), -5.0, 5.0)
    return jnp.clip(values * column, -15.0, 15.0).astype(jnp.bfloat16)


def block_scale(own_key, dims, cuts, least, largest):
    level, own = 1.0, jax.random.fold_in(own_key, 6)
    for axis_at, blocks in cuts:
        heights = jnp.exp(jax.random.uniform(jax.random.fold_in(own, axis_at), (blocks,), jnp.float32, least / len(cuts), largest / len(cuts)))
        level = level * jnp.repeat(heights, dims[axis_at] // blocks).reshape([-1 if axis == axis_at else 1 for axis in range(len(dims))])
    return level


def gaussian(stream_key, extent, width, most, cuts=(), held_as=jnp.bfloat16):
    array = width * jax.random.normal(stream_key, extent, jnp.float32)
    if cuts:
        array = array * block_scale(stream_key, extent, cuts, -0.22, 0.18)
    return jnp.clip(array, -most, most).astype(held_as)


def setup_inputs(seed: int = 0) -> dict:
    splits = jax.random.split(jax.random.key(seed), 22)
    return {
        "tokens": draw_tokens(jax.random.fold_in(splits[21], 71), 0),
        "associative_state": gaussian(splits[1], (SEQUENCE_COUNT, MIXER_HEADS, HEAD, HEAD), 0.3, 2.0, ((0, 8), (1, 4)), jnp.float32),
        "sudden_extra_decay": jnp.clip(-0.7 + 0.7 * jax.random.uniform(splits[2], (SEQUENCE_COUNT, MIXER_HEADS), jnp.float32) ** block_scale(splits[2], (SEQUENCE_COUNT, MIXER_HEADS), ((0, 8), (1, 4)), -0.2, 0.2), -0.7, 0.0),
        "head_decay_speed": jnp.clip(jnp.exp(math.log(2.0) - 3.6888794 * jax.random.uniform(splits[3], (MIXER_HEADS,), jnp.float32) ** block_scale(splits[3], (MIXER_HEADS,), ((0, 4),), -0.2, 0.2)), 0.05, 2.0),
        "opening_norm_gain": jnp.clip(1.0 + 0.18 * jax.random.normal(splits[4], (D,), jnp.float32), 0.1, 1.9),
        "opening_gate_weight": gaussian(splits[5], (D, FF), D ** -0.5, 0.109375, ((0, 4), (1, 8))),
        "opening_up_weight": gaussian(splits[6], (D, FF), D ** -0.5, 0.109375, ((0, 4), (1, 8))),
        "opening_down_weight": gaussian(splits[7], (FF, D), (FF // 16) ** -0.5, 0.25, ((0, 8), (1, 4))),
        "mixer_norm_gain": jnp.clip(1.0 + 0.18 * jax.random.normal(splits[8], (D,), jnp.float32), 0.1, 1.9),
        "query_matrix": gaussian(splits[9], (D, MIXER_HEADS * HEAD), D ** -0.5, 0.109375, ((0, 4),)),
        "key_matrix": gaussian(splits[10], (D, MIXER_HEADS * HEAD), D ** -0.5, 0.109375, ((0, 4),)),
        "value_matrix": gaussian(splits[11], (D, MIXER_HEADS * HEAD), D ** -0.5, 0.109375, ((0, 4),)),
        "output_gate_matrix": gaussian(splits[12], (D, MIXER_HEADS * HEAD), D ** -0.5, 0.109375, ((0, 4),)),
        "strength_weight": gaussian(splits[13], (D, MIXER_HEADS), D ** -0.5, 0.109375, ((0, 4),)),
        "decay_matrix": gaussian(splits[14], (D, MIXER_HEADS), D ** -0.5, 0.109375, ((0, 4),)),
        "head_read_gain": jnp.clip(1.0 + 0.18 * jax.random.normal(splits[15], (HEAD,), jnp.float32), 0.1, 1.9),
        "output_matrix": gaussian(splits[16], (MIXER_HEADS * HEAD, D), (MIXER_HEADS * HEAD) ** -0.5, 0.125, ((0, 4),)),
        "closing_norm_gain": jnp.clip(1.0 + 0.18 * jax.random.normal(splits[17], (D,), jnp.float32), 0.1, 1.9),
        "closing_gate_weight": gaussian(splits[18], (D, FF), D ** -0.5, 0.109375, ((0, 4), (1, 8))),
        "closing_up_weight": gaussian(splits[19], (D, FF), D ** -0.5, 0.109375, ((0, 4), (1, 8))),
        "closing_down_weight": gaussian(splits[20], (FF, D), (FF // 16) ** -0.5, 0.25, ((0, 8), (1, 4))),
    }


norm_eps = 1e-06

def feed_forward(resid, rows_in, gain, gate_proj, lift_proj, down_proj):
    values = rows_in.astype(jnp.float32)
    scale_of_norm = lax.rsqrt(lax.optimization_barrier(jnp.mean(values * values, axis=1, keepdims=True)) + norm_eps)
    scaled = (values * gain).astype(jnp.bfloat16)
    gate_sum = scale_of_norm * jnp.dot(scaled, gate_proj, preferred_element_type=jnp.float32)
    lift_sum = scale_of_norm * jnp.dot(scaled, lift_proj, preferred_element_type=jnp.float32)
    hidden = (jax.nn.silu(gate_sum) * lift_sum).astype(jnp.bfloat16)
    branch = jnp.dot(hidden, down_proj, preferred_element_type=jnp.float32).astype(jnp.bfloat16)
    return resid + 0.5 * branch.astype(jnp.float32)

def block_total(inputs, weight):
    row_count = inputs.shape[0]
    group = inputs.shape[1] // N_TP
    left = inputs.reshape(row_count, N_TP, group).astype(jnp.float32)
    right = weight.reshape(N_TP, group, weight.shape[1]).astype(jnp.float32)
    partial_value = jnp.einsum('bjs,jsw->bjw', left, right).astype(jnp.bfloat16)
    partial_value = lax.optimization_barrier(partial_value)
    return lax.optimization_barrier(jnp.sum(partial_value.astype(jnp.float32), axis=1))

def unit_norm(values):
    return values * lax.rsqrt(lax.optimization_barrier(jnp.sum(values * values, axis=-1, keepdims=True)) + 1e-12)

def reference(tokens, associative_state, sudden_extra_decay, head_decay_speed, opening_norm_gain, opening_gate_weight, opening_up_weight, opening_down_weight, mixer_norm_gain, query_matrix, key_matrix, value_matrix, output_gate_matrix, strength_weight, decay_matrix, head_read_gain, output_matrix, closing_norm_gain, closing_gate_weight, closing_up_weight, closing_down_weight):
    first = feed_forward(tokens.astype(jnp.float32), tokens, opening_norm_gain, opening_gate_weight, opening_up_weight, opening_down_weight)
    scale_of_norm = lax.rsqrt(lax.optimization_barrier(jnp.mean(first * first, axis=1, keepdims=True)) + norm_eps)
    mixer_input = (first * mixer_norm_gain).astype(jnp.bfloat16)

    def heads_of(weight):
        return (scale_of_norm * block_total(mixer_input, weight)).reshape(SEQUENCE_COUNT, MIXER_HEADS, HEAD)
    query_vec = unit_norm(heads_of(query_matrix)) * HEAD ** (-0.5)
    key_vec = unit_norm(heads_of(key_matrix))
    value_vec = heads_of(value_matrix)
    gate_vec = heads_of(output_gate_matrix)
    beta = jax.nn.sigmoid(scale_of_norm * block_total(mixer_input, strength_weight))
    decay_logarithm = -head_decay_speed * jax.nn.softplus(scale_of_norm * block_total(mixer_input, decay_matrix)) + sudden_extra_decay
    kept = jnp.exp(decay_logarithm)[:, :, None, None]
    recall = jnp.einsum('bhk,bhkv->bhv', key_vec, associative_state, precision=lax.Precision.HIGHEST)
    written = (beta[:, :, None] * key_vec)[:, :, :, None]
    memory_new = kept * (associative_state - written * recall[:, :, None, :]) + written * value_vec[:, :, None, :]
    read_out = jnp.einsum('bhk,bhkv->bhv', query_vec, memory_new, precision=lax.Precision.HIGHEST)
    normed = read_out * lax.rsqrt(lax.optimization_barrier(jnp.mean(read_out * read_out, axis=-1, keepdims=True)) + norm_eps)
    normed = normed * head_read_gain * jax.nn.silu(gate_vec)
    mix_out = normed.reshape(SEQUENCE_COUNT, MIXER_HEADS * HEAD).astype(jnp.bfloat16)
    mixed = block_total(mix_out, output_matrix).astype(jnp.bfloat16)
    second = first + mixed.astype(jnp.float32)
    final = feed_forward(second, second.astype(jnp.bfloat16), closing_norm_gain, closing_gate_weight, closing_up_weight, closing_down_weight)
    return (final.astype(jnp.bfloat16), memory_new)
```

```python
import functools

import jax
import jax.numpy as jnp
from jax import lax
from jax.experimental import pallas as pl
from jax.experimental.pallas import tpu as pltpu
from jax.sharding import PartitionSpec as P

norm_eps = 1e-06
MESH = pl.DeviceIdType.MESH
F32, BF16 = jnp.float32, jnp.bfloat16
UNROLL = 16
VMEM_LIMIT = 63 * 1024 * 1024


def each(count, step):
    if count <= UNROLL:
        for i in range(count):
            step(i)
    else:

        def run(i, carry):
            step(i)
            return carry

        lax.fori_loop(0, count, run, 0)


def silu(x):
    return x * jax.nn.sigmoid(x)


def dot_t(rows, weight):
    return lax.dot_general(rows, weight, (((1,), (1,)), ((), ())), preferred_element_type=F32)


class Axis:
    def __init__(self, name, size):
        self.name, self.n, self.me = name, size, lax.axis_index(name)

    def others(self, step):
        each(self.n - 1, lambda i: step(lax.rem(self.me + (i + 1), self.n)))

    def start(self, src_of, land, sems):
        def one(peer):
            pltpu.make_async_remote_copy(
                src_ref=src_of(peer),
                dst_ref=land.at[self.me],
                send_sem=sems.at[0],
                recv_sem=sems.at[1],
                device_id={self.name: peer},
                device_id_type=MESH,
            ).start()

        self.others(one)

    def wait(self, land, sem):
        part = land.at[pl.ds(0, self.n - 1)]
        pltpu.make_async_copy(part, part, sem).wait()


def kernel(
    sizes,
    tokens,
    state_hbm,
    extra,
    speed,
    gain1,
    wg1_hbm,
    wu1_hbm,
    wd1_hbm,
    mgain,
    wq_hbm,
    wk_hbm,
    wv_hbm,
    wz_hbm,
    ws_hbm,
    wa_hbm,
    hgain,
    wo_hbm,
    gain2,
    wg2_hbm,
    wu2_hbm,
    wd2_hbm,
    out,
    new_hbm,
    wg1,
    wu1,
    wd1,
    wq,
    wk,
    wv,
    wz,
    ws,
    wa,
    wo,
    wg2,
    wu2,
    wd2,
    state,
    new,
    u_land,
    rows_scr,
    gate_send,
    gate_land,
    up_send,
    up_land,
    sq_send,
    sq_land,
    hid_send,
    hid_land,
    hid_scr,
    part_send,
    part_land,
    proj_send,
    proj_land,
    small_send,
    small_land,
    mix_send,
    mix_land,
    second_send,
    pair,
    turn,
    head_out,
    load_sem,
    new_sem,
    kv_sem,
    tp_sem,
):
    n_kv, n_tp, heads, head = sizes
    kv, tp = Axis("kv", n_kv), Axis("tp", n_tp)
    rows, width = tokens.shape
    all_rows = rows * n_kv
    group = all_rows // n_tp
    model_width = width * n_tp
    own_width = heads * head
    pairs = rows * heads

    hbm = (wg1_hbm, wu1_hbm, wd1_hbm, wq_hbm, wk_hbm, wv_hbm, wz_hbm, ws_hbm, wa_hbm, state_hbm, wo_hbm, wg2_hbm, wu2_hbm, wd2_hbm)
    local = (wg1, wu1, wd1, wq, wk, wv, wz, ws, wa, state, wo, wg2, wu2, wd2)
    loads = [pltpu.make_async_copy(a, b, load_sem.at[i]) for i, (a, b) in enumerate(zip(hbm, local))]

    barrier = pltpu.get_barrier_semaphore()
    for axis in (kv, tp):
        axis.others(
            lambda peer, axis=axis: pl.semaphore_signal(
                barrier, inc=1, device_id={axis.name: peer}, device_id_type=MESH
            )
        )
    for load in loads:
        load.start()

    pair[...] = jnp.zeros_like(pair)
    turn[...] = jnp.zeros_like(turn)
    for h in range(heads):
        pair[4, rows * h : rows * (h + 1), 0:heads] = extra[...]
    lane = lax.broadcasted_iota(jnp.int32, (pairs, 128), 1)
    head_of = lax.broadcasted_iota(jnp.int32, (pairs, 128), 0) // rows
    own_lane = lane == head_of
    extra_col = jnp.sum(jnp.where(own_lane, pair[4, 0:pairs, 0:128], 0.0), axis=1, keepdims=True)
    pair[5, 0:pairs, 0:heads] = jnp.broadcast_to(speed[...], (pairs, heads))
    speed_col = jnp.sum(jnp.where(own_lane, pair[5, 0:pairs, 0:128], 0.0), axis=1, keepdims=True)

    pl.semaphore_wait(barrier, n_kv - 1 + n_tp - 1)

    def feed_forward(index, resid, src, gain, gate_w, up_w, down_w, load_at):
        land = u_land.at[index]
        kv.start(lambda peer: src, land, kv_sem.at[2 * index])
        u_land[index, kv.me] = src[...]
        kv.wait(land, kv_sem.at[2 * index, 1])

        def place(i):
            rows_scr[rows * i : rows * (i + 1), :] = u_land[index, i].astype(F32)

        for i in range(n_kv):
            place(i)
        values = rows_scr[...]
        scaled = (values * gain[...]).astype(BF16)
        square = jnp.sum(values * values, axis=1, keepdims=True)
        for t in range(n_tp):
            sq_send[index, t] = jnp.broadcast_to(square[group * t : group * (t + 1)], (group, 128))
        tp.start(lambda peer: sq_send.at[index, peer], sq_land.at[index], tp_sem.at[index, 0])
        for place_at, weight, send, landing in ((0, gate_w, gate_send, gate_land), (1, up_w, up_send, up_land)):
            loads[load_at + place_at].wait()
            product = dot_t(scaled, weight[...])
            for t in range(n_tp):
                send[index, t] = product[group * t : group * (t + 1)].astype(BF16)
            tp.start(lambda peer: send.at[index, peer], landing.at[index], tp_sem.at[index, 1 + place_at])

        def total(send, landing, sem):
            landing[index, tp.me] = send[index, tp.me]
            tp.wait(landing.at[index], sem)
            result = landing[index, 0].astype(F32)
            for t in range(1, n_tp):
                result = result + landing[index, t].astype(F32)
            return result

        square = total(sq_send, sq_land, tp_sem.at[index, 0, 1])
        scale = lax.rsqrt(square[:, 0:1] / model_width + norm_eps)
        gate = scale * total(gate_send, gate_land, tp_sem.at[index, 1, 1])
        up = scale * total(up_send, up_land, tp_sem.at[index, 2, 1])
        hidden = (silu(gate) * up).astype(BF16)
        hid_send[index] = hidden
        tp.start(lambda peer: hid_send.at[index], hid_land.at[index], tp_sem.at[index, 3])
        hid_land[index, tp.me] = hidden
        loads[load_at + 2].wait()
        tp.wait(hid_land.at[index], tp_sem.at[index, 3, 1])
        for t in range(n_tp):
            hid_scr[group * t : group * (t + 1), :] = hid_land[index, t].astype(F32)
        rows_scr[...] = jnp.dot(hid_scr[...].astype(BF16), down_w[...], preferred_element_type=F32)

        def cut(i):
            part_send[index, i] = rows_scr[rows * i : rows * (i + 1), :].astype(BF16)

        for i in range(n_kv):
            cut(i)
        kv.start(lambda peer: part_send.at[index, peer], part_land.at[index], kv_sem.at[2 * index + 1])
        part_land[index, kv.me] = part_send[index, kv.me]
        kv.wait(part_land.at[index], kv_sem.at[2 * index + 1, 1])
        if n_kv <= UNROLL:
            branch = part_land[index, 0].astype(F32)
            for i in range(1, n_kv):
                branch = branch + part_land[index, i].astype(F32)
        else:
            branch = lax.fori_loop(
                0, n_kv, lambda i, c: c + part_land[index, i].astype(F32), jnp.zeros((rows, width), F32)
            )
        return resid + 0.5 * branch.astype(BF16).astype(F32)

    first = feed_forward(0, tokens[...].astype(F32), tokens, gain1, wg1, wu1, wd1, 0)

    mixer_in = (first * mgain[...]).astype(BF16)
    square = jnp.sum(first * first, axis=1, keepdims=True)
    for w, weight in enumerate((wq, wk, wv, wz)):
        loads[3 + w].wait()
        product = jnp.dot(mixer_in, weight[...], preferred_element_type=F32)
        for t in range(n_tp):
            proj_send[w, t] = product[:, own_width * t : own_width * (t + 1)].astype(BF16)
        tp.start(lambda peer: proj_send.at[w, peer], proj_land.at[w], tp_sem.at[2, w])
    loads[7].wait()
    loads[8].wait()
    all_heads = ws.shape[0]
    small_send[...] = jnp.zeros_like(small_send)
    small_send[:, 0:all_heads] = dot_t(mixer_in, ws[...])
    small_send[:, 128 : 128 + all_heads] = dot_t(mixer_in, wa[...])
    small_send[:, 256:384] = jnp.broadcast_to(square, (rows, 128))
    tp.start(lambda peer: small_send, small_land, tp_sem.at[3, 0])
    small_land[tp.me] = small_send[...]
    for w in range(4):
        proj_land[w, tp.me] = proj_send[w, tp.me]
    loads[9].wait()
    loads[10].wait()
    for w in range(4):
        tp.wait(proj_land.at[w], tp_sem.at[2, w, 1])
    tp.wait(small_land, tp_sem.at[3, 0, 1])
    small = small_land[0]
    for t in range(1, n_tp):
        small = small + small_land[t]
    scale = lax.rsqrt(small[:, 256:257] / model_width + norm_eps)
    small = scale * small
    for w in range(4):
        value = proj_land[w, 0].astype(F32)
        for t in range(1, n_tp):
            value = value + proj_land[w, t].astype(F32)
        value = scale * value
        for h in range(heads):
            pair[w, rows * h : rows * (h + 1), :] = value[:, head * h : head * (h + 1)]
    for h in range(heads):
        pair[4, rows * h : rows * (h + 1), 0:128] = small[:, 0:128]
        pair[5, rows * h : rows * (h + 1), 0:128] = small[:, 128:256]
    my_lane = lane == head_of + heads * tp.me
    beta = jax.nn.sigmoid(jnp.sum(jnp.where(my_lane, pair[4, 0:pairs, 0:128], 0.0), axis=1, keepdims=True))
    decay = jnp.sum(jnp.where(my_lane, pair[5, 0:pairs, 0:128], 0.0), axis=1, keepdims=True)
    softplus = jnp.maximum(decay, 0.0) + jnp.log1p(jnp.exp(-jnp.abs(decay)))
    kept = jnp.exp(extra_col - speed_col * softplus)
    query, key = pair[0, 0:pairs, :], pair[1, 0:pairs, :]
    query = query * lax.rsqrt(jnp.sum(query * query, axis=1, keepdims=True) + 1e-12) * head ** (-0.5)
    key = key * lax.rsqrt(jnp.sum(key * key, axis=1, keepdims=True) + 1e-12)
    value, gate = pair[2, 0:pairs, :], pair[3, 0:pairs, :]
    overlap = jnp.sum(query * key, axis=1, keepdims=True)
    turn[0:pairs, :] = key
    turn[pairs : 2 * pairs, :] = query
    columns = jnp.transpose(turn[...])
    for p in range(pairs):
        h, r = p // rows, p % rows
        block = state[r, h]
        key_col, query_col = columns[:, p : p + 1], columns[:, pairs + p : pairs + p + 1]
        keep = kept[p : p + 1]
        recall = jnp.sum(key_col * block, axis=0, keepdims=True)
        seen = jnp.sum(query_col * block, axis=0, keepdims=True)
        delta = beta[p : p + 1] * (value[p : p + 1] - keep * recall)
        new[r, h] = keep * block + key_col * delta
        pair[6, p : p + 1, :] = keep * seen + overlap[p : p + 1] * delta
    save = pltpu.make_async_copy(new, new_hbm, new_sem)
    save.start()
    read = pair[6, 0:pairs, :]
    normed = read * lax.rsqrt(jnp.mean(read * read, axis=1, keepdims=True) + norm_eps)
    pair[6, 0:pairs, :] = normed * hgain[...] * silu(gate)
    for h in range(heads):
        head_out[:, head * h : head * (h + 1)] = pair[6, rows * h : rows * (h + 1), :]
    product = jnp.dot(head_out[...].astype(BF16), wo[...], preferred_element_type=F32)
    for t in range(n_tp):
        mix_send[t] = product[:, width * t : width * (t + 1)].astype(BF16)
    tp.start(lambda peer: mix_send.at[peer], mix_land, tp_sem.at[3, 1])
    mix_land[tp.me] = mix_send[tp.me]
    tp.wait(mix_land, tp_sem.at[3, 1, 1])
    mixed = mix_land[0].astype(F32)
    for t in range(1, n_tp):
        mixed = mixed + mix_land[t].astype(F32)
    second = first + mixed.astype(BF16).astype(F32)
    second_send[...] = second.astype(BF16)

    final = feed_forward(1, second, second_send, gain2, wg2, wu2, wd2, 11)
    out[...] = final.astype(BF16)

    save.wait()
    for index in range(2):
        kv.wait(u_land.at[index], kv_sem.at[2 * index, 0])
        kv.wait(part_land.at[index], kv_sem.at[2 * index + 1, 0])
        for i, landing in enumerate((sq_land, gate_land, up_land, hid_land)):
            tp.wait(landing.at[index], tp_sem.at[index, i, 0])
    for w in range(4):
        tp.wait(proj_land.at[w], tp_sem.at[2, w, 0])
    tp.wait(small_land, tp_sem.at[3, 0, 0])
    tp.wait(mix_land, tp_sem.at[3, 1, 0])


def body(n_kv, n_tp, *args):
    tokens, state, extra, speed = args[:4]
    wg, wd, wq, ws, wo = args[5], args[7], args[9], args[13], args[16]
    hgain = args[15]
    rows, width = tokens.shape
    heads, head = speed.shape[0], hgain.shape[0]
    hidden = wg.shape[1]
    own_width = heads * head
    all_rows = rows * n_kv
    group = all_rows // n_tp
    pair_rows = -(-rows * heads // 8) * 8
    args = [a.reshape(1, -1) if a.ndim == 1 else a for a in args]
    for i in (5, 6, 13, 14, 18, 19):
        args[i] = args[i].T
    vmem, anywhere = pl.BlockSpec(memory_space=pltpu.VMEM), pl.BlockSpec(memory_space=pl.ANY)
    in_vmem = {0, 2, 3, 4, 8, 15, 17}
    scratch = [
        pltpu.VMEM(a.shape, a.dtype)
        for a in (args[5], args[6], args[7], *args[9:15], args[16], *args[18:21], state, state)
    ]
    scratch += [
        pltpu.VMEM((2, n_kv, rows, width), BF16),
        pltpu.VMEM((all_rows, width), F32),
        pltpu.VMEM((2, n_tp, group, hidden), BF16),
        pltpu.VMEM((2, n_tp, group, hidden), BF16),
        pltpu.VMEM((2, n_tp, group, hidden), BF16),
        pltpu.VMEM((2, n_tp, group, hidden), BF16),
        pltpu.VMEM((2, n_tp, group, 128), F32),
        pltpu.VMEM((2, n_tp, group, 128), F32),
        pltpu.VMEM((2, group, hidden), BF16),
        pltpu.VMEM((2, n_tp, group, hidden), BF16),
        pltpu.VMEM((all_rows, hidden), F32),
        pltpu.VMEM((2, n_kv, rows, width), BF16),
        pltpu.VMEM((2, n_kv, rows, width), BF16),
        pltpu.VMEM((4, n_tp, rows, own_width), BF16),
        pltpu.VMEM((4, n_tp, rows, own_width), BF16),
        pltpu.VMEM((rows, 384), F32),
        pltpu.VMEM((n_tp, rows, 384), F32),
        pltpu.VMEM((n_tp, rows, width), BF16),
        pltpu.VMEM((n_tp, rows, width), BF16),
        pltpu.VMEM((rows, width), BF16),
        pltpu.VMEM((7, pair_rows, head), F32),
        pltpu.VMEM((128, head), F32),
        pltpu.VMEM((rows, own_width), F32),
        pltpu.SemaphoreType.DMA((14,)),
        pltpu.SemaphoreType.DMA,
        pltpu.SemaphoreType.DMA((4, 2)),
        pltpu.SemaphoreType.DMA((4, 4, 2)),
    ]
    return pl.pallas_call(
        functools.partial(kernel, (n_kv, n_tp, heads, head)),
        out_shape=(
            jax.ShapeDtypeStruct(tokens.shape, BF16),
            jax.ShapeDtypeStruct(state.shape, F32),
        ),
        in_specs=[vmem if i in in_vmem else anywhere for i in range(len(args))],
        out_specs=(vmem, anywhere),
        scratch_shapes=scratch,
        compiler_params=pltpu.CompilerParams(
            collective_id=0, has_side_effects=True, vmem_limit_bytes=VMEM_LIMIT
        ),
    )(*args)


def solution(mesh):
    placed = (
        P("kv", "tp"),
        P("kv", "tp", None, None),
        P("kv", "tp"),
        P("tp"),
        P("tp"),
        P("tp", "kv"),
        P("tp", "kv"),
        P("kv", "tp"),
        P("tp"),
        P("tp", None),
        P("tp", None),
        P("tp", None),
        P("tp", None),
        P("tp", None),
        P("tp", None),
        P(),
        P("tp", None),
        P("tp"),
        P("tp", "kv"),
        P("tp", "kv"),
        P("kv", "tp"),
    )
    return jax.shard_map(
        functools.partial(body, mesh.shape["kv"], mesh.shape["tp"]),
        mesh=mesh,
        in_specs=placed,
        out_specs=(P("kv", "tp"), P("kv", "tp", None, None)),
        check_vma=False,
    )
```

```python
import functools

import jax
import jax.numpy as jnp
from jax import lax
from jax.experimental import pallas as pl
from jax.experimental.pallas import tpu as pltpu
from jax.sharding import PartitionSpec as P

norm_eps = 1e-06
MESH = pl.DeviceIdType.MESH
F32, BF16 = jnp.float32, jnp.bfloat16
UNROLL = 16
VMEM_LIMIT = 63 * 1024 * 1024


def each(count, step):
    if count <= UNROLL:
        for i in range(count):
            step(i)
    else:

        def run(i, carry):
            step(i)
            return carry

        lax.fori_loop(0, count, run, 0)


def silu(x):
    return x * jax.nn.sigmoid(x)


def dot_t(rows, weight):
    return lax.dot_general(rows, weight, (((1,), (1,)), ((), ())), preferred_element_type=F32)


class Axis:
    def __init__(self, name, size):
        self.name, self.n, self.me = name, size, lax.axis_index(name)
        self.sent = []

    def others(self, step):
        each(self.n - 1, lambda i: step(lax.rem(self.me + (i + 1), self.n)))

    def start(self, src_of, land, sems):
        def one(peer):
            pltpu.make_async_remote_copy(
                src_ref=src_of(peer),
                dst_ref=land.at[self.me],
                send_sem=sems.at[0],
                recv_sem=sems.at[1],
                device_id={self.name: peer},
                device_id_type=MESH,
            ).start()

        self.others(one)
        self.sent.append((land, sems.at[0]))

    def wait(self, land, sem):
        part = land.at[pl.ds(0, self.n - 1)]
        pltpu.make_async_copy(part, part, sem).wait()


def kernel(
    sizes,
    tokens,
    state_hbm,
    extra,
    speed,
    gain1,
    wg1_hbm,
    wu1_hbm,
    wd1_hbm,
    mgain,
    wq_hbm,
    wk_hbm,
    wv_hbm,
    wz_hbm,
    ws_hbm,
    wa_hbm,
    hgain,
    wo_hbm,
    gain2,
    wg2_hbm,
    wu2_hbm,
    wd2_hbm,
    out,
    new_hbm,
    wg1,
    wu1,
    wd1,
    wq,
    wk,
    wv,
    wz,
    ws,
    wa,
    wo,
    wg2,
    wu2,
    wd2,
    state,
    new,
    u_land,
    rows_scr,
    pair_send,
    pair_land,
    chip_send,
    chip_land,
    sq_send,
    sq_land,
    sq_chip_send,
    sq_chip_land,
    hid_scr,
    part_send,
    part_land,
    proj_send,
    proj_land,
    small_send,
    small_land,
    mix_send,
    mix_land,
    second_send,
    pair,
    turn,
    head_out,
    gains,
    load_sem,
    new_sem,
    kv_sem,
    tp_sem,
    mate_sem,
):
    n_kv, n_tp, heads, head = sizes
    kv, tp = Axis("kv", n_kv), Axis("tp", n_tp)
    rows, width = tokens.shape
    all_rows = rows * n_kv
    half = all_rows // 2
    core = lax.rem(tp.me, 2)
    mate = tp.me + 1 - 2 * core
    to_finish = []
    model_width = width * n_tp
    own_width = heads * head
    pairs = rows * heads

    hbm = (wg1_hbm, wu1_hbm, wd1_hbm, wq_hbm, wk_hbm, wv_hbm, wz_hbm, ws_hbm, wa_hbm, state_hbm, wo_hbm, wg2_hbm, wu2_hbm, wd2_hbm)
    local = (wg1, wu1, wd1, wq, wk, wv, wz, ws, wa, state, wo, wg2, wu2, wd2)
    loads = [pltpu.make_async_copy(a, b, load_sem.at[i]) for i, (a, b) in enumerate(zip(hbm, local))]

    barrier = pltpu.get_barrier_semaphore()
    for axis in (kv, tp):
        axis.others(
            lambda peer, axis=axis: pl.semaphore_signal(
                barrier, inc=1, device_id={axis.name: peer}, device_id_type=MESH
            )
        )
    for load in loads[0:2]:
        load.start()

    for i, gain in enumerate((gain1, mgain, gain2)):
        lanes = gain.shape[1]
        for j in range(gain.shape[0]):
            gains[i, :, lanes * j : lanes * (j + 1)] = gain[j : j + 1, :]
    pair[...] = jnp.zeros_like(pair)
    turn[...] = jnp.zeros_like(turn)
    for h in range(heads):
        pair[4, rows * h : rows * (h + 1), 0:heads] = extra[...]
    lane = lax.broadcasted_iota(jnp.int32, (pairs, 128), 1)
    head_of = lax.broadcasted_iota(jnp.int32, (pairs, 128), 0) // rows
    own_lane = lane == head_of
    extra_col = jnp.sum(jnp.where(own_lane, pair[4, 0:pairs, 0:128], 0.0), axis=1, keepdims=True)
    pair[5, 0:pairs, 0:heads] = jnp.broadcast_to(speed[...], (pairs, heads))
    speed_col = jnp.sum(jnp.where(own_lane, pair[5, 0:pairs, 0:128], 0.0), axis=1, keepdims=True)

    pl.semaphore_wait(barrier, n_kv - 1 + n_tp - 1)
    stages = [loads[2:5], loads[5:11], loads[11:14]]

    def next_stage():
        for load in stages.pop(0) if stages else ():
            load.start()

    def feed_forward(index, resid, src, gain, gate_w, up_w, down_w, load_at):
        land = u_land.at[index]
        kv.start(lambda peer: src, land, kv_sem.at[2 * index])
        u_land[index, kv.me] = src[...]
        next_stage()
        kv.wait(land, kv_sem.at[2 * index, 1])

        def place(i):
            rows_scr[rows * i : rows * (i + 1), :] = u_land[index, i].astype(F32)

        for i in range(n_kv):
            place(i)
        next_stage()
        values = rows_scr[...]
        scaled = (values * gain).astype(BF16)
        square = jnp.sum(values * values, axis=1, keepdims=True)
        def to_mate(which, product, send, landing):
            for c in range(2):
                send[index, which, c] = product[half * c : half * (c + 1)].astype(send.dtype)
            copy = pltpu.make_async_remote_copy(
                src_ref=send.at[index, which, 1 - core],
                dst_ref=landing.at[index, which],
                send_sem=mate_sem.at[index, which + (send is sq_send) * 2, 0],
                recv_sem=mate_sem.at[index, which + (send is sq_send) * 2, 1],
                device_id={tp.name: mate},
                device_id_type=MESH,
            )
            copy.start()
            to_finish.append(copy)
            return copy

        def to_all(which, copy, send, landing, chip_send, chip_land):
            copy.wait_recv()
            chip = send[index, which, core].astype(F32) + landing[index, which].astype(F32)
            chip_send[index, which] = chip.astype(chip_send.dtype)
            tp.start(
                lambda peer: chip_send.at[index, which],
                chip_land.at[index, which],
                tp_sem.at[index, which + (send is sq_send) * 2],
            )
            chip_land[index, which, tp.me] = chip.astype(chip_send.dtype)

        square_copy = to_mate(0, jnp.broadcast_to(square, (all_rows, 128)), sq_send, sq_land)
        loads[load_at].wait()
        gate_copy = to_mate(0, dot_t(scaled, gate_w[...]), pair_send, pair_land)
        loads[load_at + 1].wait()
        up_part = dot_t(scaled, up_w[...])
        up_copy = to_mate(1, up_part, pair_send, pair_land)
        to_all(0, square_copy, sq_send, sq_land, sq_chip_send, sq_chip_land)
        to_all(0, gate_copy, pair_send, pair_land, chip_send, chip_land)
        to_all(1, up_copy, pair_send, pair_land, chip_send, chip_land)
        next_stage()
        loads[load_at + 2].wait()
        tp.wait(sq_chip_land.at[index, 0], tp_sem.at[index, 2, 1])
        tp.wait(chip_land.at[index, 0], tp_sem.at[index, 0, 1])
        tp.wait(chip_land.at[index, 1], tp_sem.at[index, 1, 1])

        def total(landing, which, c):
            result = landing[index, which, c].astype(F32)
            for t in range(c + 2, n_tp, 2):
                result = result + landing[index, which, t].astype(F32)
            return result

        for c in range(2):
            scale = lax.rsqrt(total(sq_chip_land, 0, c)[:, 0:1] / model_width + norm_eps)
            gate, up = scale * total(chip_land, 0, c), scale * total(chip_land, 1, c)
            hid_scr[half * c : half * (c + 1), :] = silu(gate) * up
        rows_scr[...] = jnp.dot(hid_scr[...].astype(BF16), down_w[...], preferred_element_type=F32)

        def cut(i):
            part_send[index, i] = rows_scr[rows * i : rows * (i + 1), :].astype(BF16)

        for i in range(n_kv):
            cut(i)
        kv.start(lambda peer: part_send.at[index, peer], part_land.at[index], kv_sem.at[2 * index + 1])
        part_land[index, kv.me] = part_send[index, kv.me]
        kv.wait(part_land.at[index], kv_sem.at[2 * index + 1, 1])
        if n_kv <= UNROLL:
            branch = part_land[index, 0].astype(F32)
            for i in range(1, n_kv):
                branch = branch + part_land[index, i].astype(F32)
        else:
            branch = lax.fori_loop(
                0, n_kv, lambda i, c: c + part_land[index, i].astype(F32), jnp.zeros((rows, width), F32)
            )
        return resid + 0.5 * branch.astype(BF16).astype(F32)

    first = feed_forward(0, tokens[...].astype(F32), tokens, gains[0], wg1, wu1, wd1, 0)

    mixer_in = (first * gains[1]).astype(BF16)
    square = jnp.sum(first * first, axis=1, keepdims=True)
    for w, weight in enumerate((wq, wk, wv, wz)):
        loads[3 + w].wait()
        product = jnp.dot(mixer_in, weight[...], preferred_element_type=F32)
        for t in range(n_tp):
            proj_send[w, t] = product[:, own_width * t : own_width * (t + 1)].astype(BF16)
        tp.start(lambda peer: proj_send.at[w, peer], proj_land.at[w], tp_sem.at[2, w])
    loads[7].wait()
    loads[8].wait()
    all_heads = ws.shape[0]
    small_send[...] = jnp.zeros_like(small_send)
    small_send[:, 0:all_heads] = dot_t(mixer_in, ws[...])
    small_send[:, 128 : 128 + all_heads] = dot_t(mixer_in, wa[...])
    small_send[:, 256:384] = jnp.broadcast_to(square, (rows, 128))
    tp.start(lambda peer: small_send, small_land, tp_sem.at[3, 0])
    small_land[tp.me] = small_send[...]
    for w in range(4):
        proj_land[w, tp.me] = proj_send[w, tp.me]
    loads[9].wait()
    loads[10].wait()
    for w in range(4):
        tp.wait(proj_land.at[w], tp_sem.at[2, w, 1])
    tp.wait(small_land, tp_sem.at[3, 0, 1])
    small = small_land[0]
    for t in range(1, n_tp):
        small = small + small_land[t]
    scale = lax.rsqrt(small[:, 256:257] / model_width + norm_eps)
    small = scale * small
    for w in range(4):
        value = proj_land[w, 0].astype(F32)
        for t in range(1, n_tp):
            value = value + proj_land[w, t].astype(F32)
        value = scale * value
        for h in range(heads):
            pair[w, rows * h : rows * (h + 1), :] = value[:, head * h : head * (h + 1)]
    for h in range(heads):
        pair[4, rows * h : rows * (h + 1), 0:128] = small[:, 0:128]
        pair[5, rows * h : rows * (h + 1), 0:128] = small[:, 128:256]
    my_lane = lane == head_of + heads * tp.me
    beta = jax.nn.sigmoid(jnp.sum(jnp.where(my_lane, pair[4, 0:pairs, 0:128], 0.0), axis=1, keepdims=True))
    decay = jnp.sum(jnp.where(my_lane, pair[5, 0:pairs, 0:128], 0.0), axis=1, keepdims=True)
    softplus = jnp.maximum(decay, 0.0) + jnp.log1p(jnp.exp(-jnp.abs(decay)))
    kept = jnp.exp(extra_col - speed_col * softplus)
    query, key = pair[0, 0:pairs, :], pair[1, 0:pairs, :]
    query = query * lax.rsqrt(jnp.sum(query * query, axis=1, keepdims=True) + 1e-12) * head ** (-0.5)
    key = key * lax.rsqrt(jnp.sum(key * key, axis=1, keepdims=True) + 1e-12)
    value, gate = pair[2, 0:pairs, :], pair[3, 0:pairs, :]
    overlap = jnp.sum(query * key, axis=1, keepdims=True)
    turn[0:pairs, :] = key
    turn[pairs : 2 * pairs, :] = query
    columns = jnp.transpose(turn[...])
    for p in range(pairs):
        h, r = p // rows, p % rows
        block = state[r, h]
        key_col, query_col = columns[:, p : p + 1], columns[:, pairs + p : pairs + p + 1]
        keep = kept[p : p + 1]
        recall = jnp.sum(key_col * block, axis=0, keepdims=True)
        seen = jnp.sum(query_col * block, axis=0, keepdims=True)
        delta = beta[p : p + 1] * (value[p : p + 1] - keep * recall)
        new[r, h] = keep * block + key_col * delta
        pair[6, p : p + 1, :] = keep * seen + overlap[p : p + 1] * delta
    save = pltpu.make_async_copy(new, new_hbm, new_sem)
    save.start()
    read = pair[6, 0:pairs, :]
    normed = read * lax.rsqrt(jnp.mean(read * read, axis=1, keepdims=True) + norm_eps)
    pair[6, 0:pairs, :] = normed * hgain[...] * silu(gate)
    for h in range(heads):
        head_out[:, head * h : head * (h + 1)] = pair[6, rows * h : rows * (h + 1), :]
    product = jnp.dot(head_out[...].astype(BF16), wo[...], preferred_element_type=F32)
    for t in range(n_tp):
        mix_send[t] = product[:, width * t : width * (t + 1)].astype(BF16)
    tp.start(lambda peer: mix_send.at[peer], mix_land, tp_sem.at[3, 1])
    mix_land[tp.me] = mix_send[tp.me]
    tp.wait(mix_land, tp_sem.at[3, 1, 1])
    mixed = mix_land[0].astype(F32)
    for t in range(1, n_tp):
        mixed = mixed + mix_land[t].astype(F32)
    second = first + mixed.astype(BF16).astype(F32)
    second_send[...] = second.astype(BF16)

    final = feed_forward(1, second, second_send, gains[2], wg2, wu2, wd2, 11)
    out[...] = final.astype(BF16)

    save.wait()
    for copy in to_finish:
        copy.wait_send()
    for axis in (kv, tp):
        for landing, sem in axis.sent:
            axis.wait(landing, sem)


def hand_over(out_in, new_in, out, new, held, in_sem, out_sem):
    reads = [pltpu.make_async_copy(new_in.at[r], held.at[r], in_sem.at[r]) for r in range(held.shape[0])]
    writes = [pltpu.make_async_copy(held.at[r], new.at[r], out_sem.at[r]) for r in range(held.shape[0])]
    for read in reads:
        read.start()
    out[...] = out_in[...]
    for read, write in zip(reads, writes):
        read.wait()
        write.start()
    for write in writes:
        write.wait()


def body(n_kv, n_tp, *args):
    tokens, state, extra, speed = args[:4]
    wg, wd, wq, ws, wo = args[5], args[7], args[9], args[13], args[16]
    hgain = args[15]
    rows, width = tokens.shape
    heads, head = speed.shape[0], hgain.shape[0]
    hidden = wg.shape[1]
    own_width = heads * head
    all_rows = rows * n_kv
    half = all_rows // 2
    pair_rows = -(-rows * heads // 8) * 8
    args = [a.reshape(-1, 128 if a.size % 128 == 0 else a.size) if a.ndim == 1 else a for a in args]
    for i in (5, 6, 13, 14, 18, 19):
        args[i] = args[i].T
    vmem, anywhere = pl.BlockSpec(memory_space=pltpu.VMEM), pl.BlockSpec(memory_space=pl.ANY)
    in_vmem = {0, 2, 3, 4, 8, 15, 17}
    scratch = [
        pltpu.VMEM(a.shape, a.dtype)
        for a in (args[5], args[6], args[7], *args[9:15], args[16], *args[18:21], state, state)
    ]
    scratch += [
        pltpu.VMEM((2, n_kv, rows, width), BF16),
        pltpu.VMEM((all_rows, width), F32),
        pltpu.VMEM((2, 2, 2, half, hidden), BF16),
        pltpu.VMEM((2, 2, half, hidden), BF16),
        pltpu.VMEM((2, 2, half, hidden), BF16),
        pltpu.VMEM((2, 2, n_tp, half, hidden), BF16),
        pltpu.VMEM((2, 1, 2, half, 128), F32),
        pltpu.VMEM((2, 1, half, 128), F32),
        pltpu.VMEM((2, 1, half, 128), F32),
        pltpu.VMEM((2, 1, n_tp, half, 128), F32),
        pltpu.VMEM((all_rows, hidden), F32),
        pltpu.VMEM((2, n_kv, rows, width), BF16),
        pltpu.VMEM((2, n_kv, rows, width), BF16),
        pltpu.VMEM((4, n_tp, rows, own_width), BF16),
        pltpu.VMEM((4, n_tp, rows, own_width), BF16),
        pltpu.VMEM((rows, 384), F32),
        pltpu.VMEM((n_tp, rows, 384), F32),
        pltpu.VMEM((n_tp, rows, width), BF16),
        pltpu.VMEM((n_tp, rows, width), BF16),
        pltpu.VMEM((rows, width), BF16),
        pltpu.VMEM((7, pair_rows, head), F32),
        pltpu.VMEM((128, head), F32),
        pltpu.VMEM((rows, own_width), F32),
        pltpu.VMEM((3, 1, width), F32),
        pltpu.SemaphoreType.DMA((14,)),
        pltpu.SemaphoreType.DMA,
        pltpu.SemaphoreType.DMA((4, 2)),
        pltpu.SemaphoreType.DMA((4, 4, 2)),
        pltpu.SemaphoreType.DMA((2, 3, 2)),
    ]
    out, new = pl.pallas_call(
        functools.partial(kernel, (n_kv, n_tp, heads, head)),
        out_shape=(
            jax.ShapeDtypeStruct(tokens.shape, BF16),
            jax.ShapeDtypeStruct(state.shape, F32),
        ),
        in_specs=[vmem if i in in_vmem else anywhere for i in range(len(args))],
        out_specs=(vmem, anywhere),
        scratch_shapes=scratch,
        compiler_params=pltpu.CompilerParams(
            collective_id=0, has_side_effects=True, vmem_limit_bytes=VMEM_LIMIT
        ),
    )(*args)
    return pl.pallas_call(
        hand_over,
        out_shape=(
            jax.ShapeDtypeStruct(tokens.shape, BF16),
            jax.ShapeDtypeStruct(state.shape, F32),
        ),
        in_specs=[vmem, anywhere],
        out_specs=(vmem, anywhere),
        scratch_shapes=[
            pltpu.VMEM(state.shape, F32),
            pltpu.SemaphoreType.DMA((rows,)),
            pltpu.SemaphoreType.DMA((rows,)),
        ],
        compiler_params=pltpu.CompilerParams(vmem_limit_bytes=VMEM_LIMIT),
    )(out, new)


def solution(mesh):
    placed = (
        P("kv", "tp"),
        P("kv", "tp", None, None),
        P("kv", "tp"),
        P("tp"),
        P("tp"),
        P("tp", "kv"),
        P("tp", "kv"),
        P("kv", "tp"),
        P("tp"),
        P("tp", None),
        P("tp", None),
        P("tp", None),
        P("tp", None),
        P("tp", None),
        P("tp", None),
        P(),
        P("tp", None),
        P("tp"),
        P("tp", "kv"),
        P("tp", "kv"),
        P("kv", "tp"),
    )
    return jax.shard_map(
        functools.partial(body, mesh.shape["kv"], mesh.shape["tp"]),
        mesh=mesh,
        in_specs=placed,
        out_specs=(P("kv", "tp"), P("kv", "tp", None, None)),
        check_vma=False,
    )
```
